32 devices in a mesh: fs: 4 (over z), tp: 8 (over y, x, core).
Axes of the slice: x: 2, y: 2, z: 4, core: 2. Of those that a mesh axis runs over, the one named last changes fastest.
Arguments:
- grad_gate: float32 [2112, 5632], P('fs', 'tp'), may hold values from -45 to 45
- grad_up: float32 [2112, 5632], P('fs', 'tp'), may hold values from -45 to 45
- moment_gate: float32 [2112, 5632], P('fs', 'tp'), may hold values from -6 to 6
- moment_up: float32 [2112, 5632], P('fs', 'tp'), may hold values from -6 to 6
Outputs:
- moment_gate_next: float32 [2112, 5632], P('fs', 'tp')
- moment_up_next: float32 [2112, 5632], P('fs', 'tp')
- update_gate: float32 [2112, 5632], P('fs', 'tp')
- update_up: float32 [2112, 5632], P('fs', 'tp')
The draws below stay inside these ranges and needn't reach their ends.
All inputs are finite; a program needn't handle non-finite values.
Results may differ from the reference program's by a relative error of at most 0.0019.
The reference program's roundings to bfloat16 on the way (of `poly_low` and `product_low`) count: a program that leaves them out, or rounds other values in their place, can miss the bound.
Values may be sent and summed in bfloat16 or wider, within the bound.
A program may use at most 64 MiB of HBM per device.

```python
import math
import jax
import jax.numpy as jnp

D = 2112
FF = 5632
ITERS = 3


def scaled_noise(key):
    key_rows, key_cols, key_base = jax.random.split(key, 3)
    row_scales = jnp.exp(jax.random.uniform(key_rows, (D, 1), jnp.float32, 0.0, math.log(10.0)))
    col_scales = jnp.exp(jax.random.uniform(key_cols, (1, FF), jnp.float32, 0.0, math.log(3.0)))
    base = jnp.clip(jax.random.normal(key_base, (D, FF), jnp.float32), -6.0, 6.0)
    return base * row_scales * col_scales / 4.0


def draw_grad_gate(key, part):
    return scaled_noise(jax.random.fold_in(key, 11))


def draw_grad_up(key, part):
    return scaled_noise(jax.random.fold_in(key, 23))


def block_levels(key, shape, pieces, least, high):
    factor_of = 1.0
    for axis_at, parts in pieces:
        steps = jax.random.uniform(jax.random.fold_in(jax.random.fold_in(key, 6), axis_at), (parts,), jnp.float32, least / len(pieces), high / len(pieces))
        factor_of = factor_of * jnp.repeat(jnp.exp(steps), shape[axis_at] // parts).reshape((-1,) + (1,) * (len(shape) - 1 - axis_at))
    return factor_of


def normal_values(own_key, shape, width, bound, cuts=(), held_as=jnp.bfloat16):
    drawn = width * jax.random.normal(own_key, shape, jnp.float32)
    if cuts:
        drawn = drawn * block_levels(own_key, shape, cuts, -0.22, 0.18)
    return jnp.clip(drawn, -bound, bound).astype(held_as)


def setup_inputs(seed: int = 0) -> dict:
    arg_keys = jax.random.split(jax.random.key(seed), 5)
    grad_gate = draw_grad_gate(jax.random.fold_in(arg_keys[4], 71), 0)
    grad_up = draw_grad_up(jax.random.fold_in(arg_keys[4], 71), 0)
    moment_gate = normal_values(arg_keys[2], (D, FF), 1.0, 6.0, ((0, 4), (1, 8)), jnp.float32)
    moment_up = normal_values(arg_keys[3], (D, FF), 1.0, 6.0, ((0, 4), (1, 8)), jnp.float32)
    return {"grad_gate": grad_gate, "grad_up": grad_up, "moment_gate": moment_gate, "moment_up": moment_up}


BETA = 0.95
EPS = 1e-06

def reference(grad_gate, grad_up, moment_gate, moment_up):
    moment_gate_next = BETA * moment_gate + grad_gate
    moment_up_next = BETA * moment_up + grad_up
    low_gate = moment_gate_next.astype(jnp.bfloat16)
    low_up = moment_up_next.astype(jnp.bfloat16)
    gram = jnp.dot(low_gate, low_gate.T, preferred_element_type=jnp.float32) + jnp.dot(low_up, low_up.T, preferred_element_type=jnp.float32)
    trace_total = jnp.sum(jnp.square(low_gate.astype(jnp.float32))) + jnp.sum(jnp.square(low_up.astype(jnp.float32)))
    square_total = jnp.sum(gram * gram)
    spectral = 2.0 * square_total / (trace_total + EPS)
    current = gram / spectral
    identity = jnp.eye(D, dtype=jnp.float32)
    product_low = None
    for iteration in range(ITERS):
        poly_low = (1.5 * identity - 0.5 * current).astype(jnp.bfloat16)
        if iteration == 0:
            product_low = poly_low
        else:
            product_low = jnp.dot(product_low, poly_low, preferred_element_type=jnp.float32).astype(jnp.bfloat16)
        if iteration < ITERS - 1:
            square_low = jnp.dot(poly_low, poly_low, preferred_element_type=jnp.float32).astype(jnp.bfloat16)
            current = jnp.dot(current.astype(jnp.bfloat16), square_low, preferred_element_type=jnp.float32)
    factor = jnp.sqrt(2.0 * FF / spectral)
    update_gate = jnp.dot(product_low.T, low_gate, preferred_element_type=jnp.float32) * factor
    update_up = jnp.dot(product_low.T, low_up, preferred_element_type=jnp.float32) * factor
    return (moment_gate_next, moment_up_next, update_gate, update_up)
```

```python
import functools

import jax
import jax.numpy as jnp
from jax import lax
from jax.experimental import pallas as pl
from jax.experimental.pallas import tpu as pltpu
from jax.sharding import PartitionSpec as P

ITERS = 3


BETA = 0.95
EPS = 1e-06


def multiply(left_low, right_low):
    left_rows = lax.all_gather(left_low, "fs", axis=1, tiled=True)
    return jnp.dot(
        left_rows,
        lax.all_gather(right_low, "tp", axis=0, tiled=True),
        preferred_element_type=jnp.float32,
    )


def local_small(grad_gate, grad_up, moment_gate, moment_up):
    hidden = grad_gate.shape[1] * lax.axis_size("tp")
    moment_gate_next = BETA * moment_gate + grad_gate
    moment_up_next = BETA * moment_up + grad_up
    low_gate = moment_gate_next.astype(jnp.bfloat16)
    low_up = moment_up_next.astype(jnp.bfloat16)
    trace_local = jnp.sum(jnp.square(low_gate.astype(jnp.float32))) + jnp.sum(
        jnp.square(low_up.astype(jnp.float32))
    )
    columns_gate, columns_up = (
        lax.all_gather(low_gate, "fs", axis=0, tiled=True),
        lax.all_gather(low_up, "fs", axis=0, tiled=True),
    )
    rows_dev = low_gate.shape[0]
    width = columns_gate.shape[0]
    own_rows = width // lax.axis_size("tp")
    block_gate = columns_gate
    block_up = columns_up
    gram = lax.psum_scatter(
        jnp.einsum("ik,jk->ij", block_gate, low_gate, preferred_element_type=jnp.float32)
        + jnp.einsum("ik,jk->ij", block_up, low_up, preferred_element_type=jnp.float32),
        "tp",
        scatter_dimension=0,
        tiled=True,
    )
    square_local = jnp.sum(gram * gram)
    trace_total, square_total = lax.psum((trace_local, square_local), ("fs", "tp"))
    spectral = 2.0 * square_total / (trace_total + EPS)
    current = gram / spectral
    row_index = lax.axis_index("tp") * own_rows + lax.broadcasted_iota(
        jnp.int32, (own_rows, rows_dev), 0
    )
    col_index = lax.axis_index("fs") * rows_dev + lax.broadcasted_iota(
        jnp.int32, (own_rows, rows_dev), 1
    )
    identity = (row_index == col_index).astype(jnp.float32)
    product_low = None
    for iteration in range(ITERS):
        poly_low = (1.5 * identity - 0.5 * current).astype(jnp.bfloat16)
        final_turn = iteration == ITERS - 1
        square_low = None
        if iteration == 0:
            product_low = poly_low
            square_low = multiply(poly_low, poly_low).astype(jnp.bfloat16)
        elif final_turn:
            product_low = multiply(product_low, poly_low).astype(jnp.bfloat16)
        else:
            product_low = multiply(product_low, poly_low).astype(jnp.bfloat16)
            square_low = multiply(poly_low, poly_low).astype(jnp.bfloat16)
        if not final_turn:
            current = multiply(current.astype(jnp.bfloat16), square_low)
    factor = jnp.sqrt(2.0 * hidden / spectral)
    segment = lax.all_gather(product_low, "tp", axis=0, tiled=True)
    block_gate = columns_gate
    block_up = columns_up
    ortho_gate = jnp.einsum("jr,jc->rc", segment, block_gate, preferred_element_type=jnp.float32)
    ortho_up = jnp.einsum("jr,jc->rc", segment, block_up, preferred_element_type=jnp.float32)
    return (moment_gate_next, moment_up_next, ortho_gate * factor, ortho_up * factor)


MESH = pl.DeviceIdType.MESH


def remote(src, dst, send_sem, recv_sem, z, t):
    return pltpu.make_async_remote_copy(
        src_ref=src,
        dst_ref=dst,
        send_sem=send_sem,
        recv_sem=recv_sem,
        device_id=(z, t),
        device_id_type=MESH,
    )


def gather_kernel(
    planes, ranks, low_ref, vec_ref, cols_ref, gram_ref, vecs_ref, z_send, z_recv, v_send, v_recv
):
    z, t = lax.axis_index("fs"), lax.axis_index("tp")
    offsets = [(a, b) for a in range(planes) for b in range(ranks) if a or b]
    barrier = pltpu.get_barrier_semaphore()
    for a, b in offsets:
        pl.semaphore_signal(
            barrier,
            inc=1,
            device_id=(lax.rem(z + a, planes), lax.rem(t + b, ranks)),
            device_id_type=MESH,
        )
    pl.semaphore_wait(barrier, len(offsets))

    def right(step):
        block = z - step
        src = low_ref if step == 0 else cols_ref.at[block]
        copy = remote(src, cols_ref.at[block], z_send.at[0, step], z_recv.at[0, step], z + 1, t)
        return copy, (block >= 0) & (z + 1 < planes)

    def left(step):
        block = z + step
        src = low_ref if step == 0 else cols_ref.at[block]
        copy = remote(src, cols_ref.at[block], z_send.at[1, step], z_recv.at[1, step], z - 1, t)
        return copy, (block < planes) & (z >= 1)

    def start(make, step):
        copy, valid = make(step)

        @pl.when(valid)
        def _():
            copy.start()

    def product(block):
        tile = 176 if low_ref.shape[0] % 176 == 0 else low_ref.shape[0]

        @pl.loop(0, low_ref.shape[0] // tile)
        def _(i):
            rows = pl.ds(pl.multiple_of(i * tile, 16), tile)
            gram_ref[block, rows, :] = lax.dot_general(
                cols_ref[block, rows, :],
                low_ref[...],
                (((1,), (1,)), ((), ())),
                preferred_element_type=jnp.float32,
            )

    start(right, 0)
    start(left, 0)
    small = []
    for a, b in offsets:
        copy = remote(
            vec_ref,
            vecs_ref.at[z, t],
            v_send.at[a, b],
            v_recv.at[a, b],
            lax.rem(z + a, planes),
            lax.rem(t + b, ranks),
        )
        copy.start()
        small.append(copy)
    vecs_ref[z, t] = vec_ref[...]
    cols_ref[z] = low_ref[...]
    product(z)
    for step in range(planes - 1):
        from_left = z - 1 - step
        from_right = z + 1 + step

        @pl.when(from_left >= 0)
        def _():
            remote(
                low_ref, cols_ref.at[from_left], z_send.at[0, step], z_recv.at[0, step], z, t
            ).wait_recv()

        if step + 1 < planes - 1:
            start(right, step + 1)

        @pl.when(from_right < planes)
        def _():
            remote(
                low_ref, cols_ref.at[from_right], z_send.at[1, step], z_recv.at[1, step], z, t
            ).wait_recv()

        if step + 1 < planes - 1:
            start(left, step + 1)

        @pl.when(from_left >= 0)
        def _():
            product(from_left)

        @pl.when(from_right < planes)
        def _():
            product(from_right)

    for make in (right, left):
        for step in range(planes - 1):
            copy, valid = make(step)

            @pl.when(valid)
            def _():
                copy.wait_send()

    for copy in small:
        copy.wait()


def gather_and_gram(low, vec, planes, ranks):
    rows, depth = low.shape
    vmem = pl.BlockSpec(memory_space=pltpu.VMEM)
    return pl.pallas_call(
        functools.partial(gather_kernel, planes, ranks),
        out_shape=(
            jax.ShapeDtypeStruct((planes, rows, depth), jnp.bfloat16),
            jax.ShapeDtypeStruct((planes, rows, rows), jnp.float32),
            jax.ShapeDtypeStruct((planes, ranks, 1, rows), jnp.float32),
        ),
        in_specs=[vmem, vmem],
        out_specs=(vmem, vmem, vmem),
        scratch_shapes=[
            pltpu.SemaphoreType.DMA((2, planes)),
            pltpu.SemaphoreType.DMA((2, planes)),
            pltpu.SemaphoreType.DMA((planes, ranks)),
            pltpu.SemaphoreType.DMA((planes, ranks)),
        ],
        compiler_params=pltpu.CompilerParams(
            collective_id=1, has_side_effects=True, vmem_limit_bytes=40 << 20
        ),
        cost_estimate=pl.CostEstimate(
            flops=2 * planes * rows * rows * depth, bytes_accessed=100 << 20, transcendentals=0
        ),
    )(low, vec)


def spread_kernel(
    planes,
    gram_ref,
    full_ref,
    halves,
    part,
    landed,
    h_send,
    h_recv,
    p_send,
    p_recv,
    z_send,
    z_recv,
    a_send,
    a_recv,
    b_send,
    b_recv,
    d_send,
    d_recv,
):
    z, t = lax.axis_index("fs"), lax.axis_index("tp")
    core, chip = lax.rem(t, 2), t // 2
    cx, cy = lax.rem(chip, 2), chip // 2
    sib = t + 1 - 2 * core
    x_peer = t + 2 * (1 - 2 * cx)
    y_peer = t + 4 * (1 - 2 * cy)
    xy_peer = t + 2 * (1 - 2 * cx) + 4 * (1 - 2 * cy)
    first = jnp.where(core == 0, x_peer, y_peer)
    second = jnp.where(core == 0, y_peer, x_peer)

    barrier = pltpu.get_barrier_semaphore()
    for peer in (sib, x_peer, y_peer, xy_peer):
        pl.semaphore_signal(barrier, inc=1, device_id=(z, peer), device_id_type=MESH)

    @pl.when(z >= 1)
    def _():
        pl.semaphore_signal(barrier, inc=1, device_id=(z - 1, t), device_id_type=MESH)

    @pl.when(z + 1 < planes)
    def _():
        pl.semaphore_signal(barrier, inc=1, device_id=(z + 1, t), device_id_type=MESH)

    ends = jnp.where(z >= 1, 1, 0) + jnp.where(z + 1 < planes, 1, 0)
    pl.semaphore_wait(barrier, 4 + ends)

    swaps = []
    for c in range(4):
        copy = remote(gram_ref.at[c, 1 - core], halves.at[c], h_send.at[c], h_recv.at[c], z, sib)
        copy.start()
        swaps.append(copy)
    for copy in swaps:
        copy.wait()
    for c in range(4):
        part[c] = (gram_ref[c, core] + halves[c]).astype(jnp.bfloat16)
    sends = []
    for k, peer in enumerate((xy_peer, x_peer, y_peer)):
        copy = remote(part.at[peer // 2], landed.at[k], p_send.at[k], p_recv.at[k], z, peer)
        copy.start()
        sends.append(copy)
    own = gram_ref[chip, core] + halves[chip]
    for copy in sends:
        copy.wait()
    for k in range(3):
        own = own + landed[k].astype(jnp.float32)
    full_ref[z, t] = own.astype(jnp.bfloat16)

    events = [(0, 0)]
    for s in range(planes - 1):
        events += [(1, s), (2, s)]

    def block_of(kind, s):
        if kind == 0:
            return z, None
        if kind == 1:
            return z - 1 - s, z - 1 - s >= 0
        return z + 1 + s, z + 1 + s < planes

    def guarded(valid, body):
        if valid is None:
            body()
        else:
            pl.when(valid)(body)

    def z_copy(direction, s):
        block = z - s if direction == 0 else z + s
        target = z + 1 if direction == 0 else z - 1
        valid = (block >= 0) & (target < planes) if direction == 0 else (block < planes) & (target >= 0)
        slot = full_ref.at[block, t]
        return remote(slot, slot, z_send.at[direction, s], z_recv.at[direction, s], target, t), valid

    def a_copy(e, block):
        slot = full_ref.at[block, t]
        return remote(slot, slot, a_send.at[e], a_recv.at[e], z, first)

    def b_copy(e, block, k):
        slot = full_ref.at[block, t if k == 0 else first]
        return remote(slot, slot, b_send.at[e, k], b_recv.at[e, k], z, second)

    third = jnp.where(core == 0, y_peer, x_peer)
    fourth = xy_peer

    def d_copy(e, block, k):
        rank = (t, first, third, fourth)[k]
        slot = full_ref.at[block, rank]
        return remote(slot, slot, d_send.at[e, k], d_recv.at[e, k], z, sib)

    def stage_a(e):
        kind, s = events[e]
        block, valid = block_of(kind, s)

        def body():
            if kind == 1:
                z_copy(0, s)[0].wait_recv()
            if kind == 2:
                z_copy(1, s)[0].wait_recv()

        guarded(valid, body)
        if kind == 0:
            for direction in (0, 1):
                copy, ok = z_copy(direction, 0)
                guarded(ok, copy.start)
        elif s + 1 < planes - 1:
            copy, ok = z_copy(kind - 1, s + 1)
            guarded(ok, copy.start)

        def sends():
            a_copy(e, block).start()
            b_copy(e, block, 0).start()
            d_copy(e, block, 0).start()

        guarded(valid, sends)

    def stage_b(e):
        block, valid = block_of(*events[e])

        def body():
            a_copy(e, block).wait_recv()
            b_copy(e, block, 1).start()
            d_copy(e, block, 1).start()

        guarded(valid, body)

    def stage_c(e):
        block, valid = block_of(*events[e])

        def body():
            b_copy(e, block, 0).wait_recv()
            d_copy(e, block, 2).start()
            b_copy(e, block, 1).wait_recv()
            d_copy(e, block, 3).start()

        guarded(valid, body)

    def stage_d(e):
        block, valid = block_of(*events[e])

        def body():
            a_copy(e, block).wait_send()
            for k in range(2):
                b_copy(e, block, k).wait_send()
            for k in range(4):
                d_copy(e, block, k).wait()

        guarded(valid, body)

    count = len(events)
    for e in range(count + 3):
        if e < count:
            stage_a(e)
        if 0 <= e - 1 < count:
            stage_b(e - 1)
        if 0 <= e - 3 < count:
            stage_c(e - 3)
    for e in range(count):
        stage_d(e)
    for direction in (0, 1):
        for s in range(planes - 1):
            copy, ok = z_copy(direction, s)
            guarded(ok, copy.wait_send)


def sum_and_spread(gram, planes):
    chips, _, rows, cols = gram.shape
    vmem = pl.BlockSpec(memory_space=pltpu.VMEM)
    events = 2 * planes - 1
    dma = pltpu.SemaphoreType.DMA
    return pl.pallas_call(
        functools.partial(spread_kernel, planes),
        out_shape=jax.ShapeDtypeStruct((planes, 2 * chips, rows, cols), jnp.bfloat16),
        in_specs=[vmem],
        out_specs=vmem,
        scratch_shapes=[
            pltpu.VMEM((chips, rows, cols), jnp.float32),
            pltpu.VMEM((chips, rows, cols), jnp.bfloat16),
            pltpu.VMEM((3, rows, cols), jnp.bfloat16),
            dma((4,)),
            dma((4,)),
            dma((3,)),
            dma((3,)),
            dma((2, planes)),
            dma((2, planes)),
            dma((events,)),
            dma((events,)),
            dma((events, 2)),
            dma((events, 2)),
            dma((events, 4)),
            dma((events, 4)),
        ],
        compiler_params=pltpu.CompilerParams(
            collective_id=2, has_side_effects=True, vmem_limit_bytes=48 << 20
        ),
        cost_estimate=pl.CostEstimate(flops=0, bytes_accessed=100 << 20, transcendentals=0),
    )(gram)


def tile_of(rows, most):
    return max(k for k in range(16, min(rows, most) + 1, 16) if rows % k == 0)


def eye_minus_half(current, first_row):
    at_row = lax.broadcasted_iota(jnp.int32, current.shape, 0) + first_row
    at_col = lax.broadcasted_iota(jnp.int32, current.shape, 1)
    return jnp.where(at_row == at_col, 1.5, 0.0) - 0.5 * current


def chain_kernel(
    rows_dev,
    current_ref,
    poly_ref,
    out_ref,
    square,
    current1,
    poly1,
    square1,
    poly2,
    s_send,
    s_recv,
    c_send,
    c_recv,
    p_send,
    p_recv,
    q_send,
    q_recv,
):
    z, t = lax.axis_index("fs"), lax.axis_index("tp")
    core = lax.rem(t, 2)
    sib = t + 1 - 2 * core
    half = current_ref.shape[0] // 2
    tile = tile_of(half, 352)
    tiles = half // tile
    base = core * half

    def rows_of(i):
        return pl.ds(pl.multiple_of(base + i * tile, 16), tile)

    def share(buffer, send, recv, i):
        rows = rows_of(i)
        return remote(buffer.at[rows], buffer.at[rows], send.at[i], recv.at[i], z, sib)

    barrier = pltpu.get_barrier_semaphore()
    pl.semaphore_signal(barrier, inc=1, device_id=(z, sib), device_id_type=MESH)
    pl.semaphore_wait(barrier, 1)

    def dot(left, right):
        return jnp.dot(left, right, preferred_element_type=jnp.float32)

    @pl.loop(0, tiles)
    def _(i):
        rows = rows_of(i)
        square[rows, :] = dot(poly_ref[rows, :], poly_ref[...]).astype(jnp.bfloat16)
        share(square, s_send, s_recv, i).start()

    for i in range(tiles):
        share(square, s_send, s_recv, i).wait()

    @pl.loop(0, tiles)
    def _(i):
        rows = rows_of(i)
        value = dot(current_ref[rows, :], square[...])
        current1[rows, :] = value.astype(jnp.bfloat16)
        poly1[rows, :] = eye_minus_half(value, base + i * tile).astype(jnp.bfloat16)
        share(poly1, p_send, p_recv, i).start()
        share(current1, c_send, c_recv, i).start()

    for i in range(tiles):
        share(poly1, p_send, p_recv, i).wait()
        share(current1, c_send, c_recv, i).wait()

    @pl.loop(0, tiles)
    def _(i):
        rows = rows_of(i)
        square[rows, :] = dot(poly_ref[rows, :], poly1[...]).astype(jnp.bfloat16)
        share(square, q_send, q_recv, i).start()

    small = tile_of(rows_dev, 176)
    offset = z * rows_dev

    @pl.loop(0, rows_dev // small)
    def _(i):
        rows = pl.ds(pl.multiple_of(offset + i * small, 16), small)
        here = pl.ds(pl.multiple_of(i * small, 16), small)
        square1[here, :] = dot(poly1[rows, :], poly1[...]).astype(jnp.bfloat16)

    @pl.loop(0, rows_dev // small)
    def _(i):
        here = pl.ds(pl.multiple_of(i * small, 16), small)
        value = dot(square1[here, :], current1[...])
        poly2[here, :] = eye_minus_half(value, offset + i * small).astype(jnp.bfloat16)

    for i in range(tiles):
        share(square, q_send, q_recv, i).wait()

    @pl.loop(0, rows_dev // small)
    def _(i):
        here = pl.ds(pl.multiple_of(i * small, 16), small)
        out_ref[here, :] = dot(poly2[here, :], square[...]).astype(jnp.bfloat16)


def chain(current_low, poly0, rows_dev):
    width = current_low.shape[0]
    vmem = pl.BlockSpec(memory_space=pltpu.VMEM)
    whole = pltpu.VMEM((width, width), jnp.bfloat16)
    strip = pltpu.VMEM((rows_dev, width), jnp.bfloat16)
    tiles = (width // 2) // tile_of(width // 2, 352)
    return pl.pallas_call(
        functools.partial(chain_kernel, rows_dev),
        out_shape=jax.ShapeDtypeStruct((rows_dev, width), jnp.bfloat16),
        in_specs=[vmem, vmem],
        out_specs=vmem,
        scratch_shapes=[whole, whole, whole, strip, strip]
        + [pltpu.SemaphoreType.DMA((tiles,))] * 8,
        compiler_params=pltpu.CompilerParams(
            collective_id=3, has_side_effects=True, vmem_limit_bytes=67043328
        ),
        cost_estimate=pl.CostEstimate(
            flops=4 * width**3, bytes_accessed=100 << 20, transcendentals=0
        ),
    )(current_low, poly0)


def local(grad_gate, grad_up, moment_gate, moment_up):
    if grad_gate.shape[0] % 16 or (2 * grad_gate.shape[1]) % 128 or lax.axis_size("tp") != 8 or (grad_gate.shape[0] * lax.axis_size("fs")) % 32:
        return local_small(grad_gate, grad_up, moment_gate, moment_up)
    hidden = grad_gate.shape[1] * lax.axis_size("tp")
    moment_gate_next = BETA * moment_gate + grad_gate
    moment_up_next = BETA * moment_up + grad_up
    low = jnp.concatenate(
        [moment_gate_next.astype(jnp.bfloat16), moment_up_next.astype(jnp.bfloat16)], axis=1
    )
    rows_dev = low.shape[0]
    row_squares = jnp.sum(jnp.square(low.astype(jnp.float32)), axis=1)
    planes, ranks = lax.axis_size("fs"), lax.axis_size("tp")
    blocks, shares, vecs = gather_and_gram(low, row_squares[None, :], planes, ranks)
    columns = blocks.reshape(planes * rows_dev, -1)
    width = planes * rows_dev
    diag_gram = jnp.sum(vecs, axis=1).reshape(width)
    spread = sum_and_spread(shares.reshape(ranks // 2, 2, width // ranks, rows_dev), planes)
    at_row = lax.broadcasted_iota(jnp.int32, spread.shape, 1) * (
        width // ranks
    ) + lax.broadcasted_iota(jnp.int32, spread.shape, 2)
    at_col = lax.broadcasted_iota(jnp.int32, spread.shape, 0) * rows_dev + (
        lax.broadcasted_iota(jnp.int32, spread.shape, 3)
    )
    square_total = jnp.sum(
        jnp.where(at_row == at_col, 0.0, jnp.square(spread.astype(jnp.float32)))
    ) + jnp.sum(jnp.square(diag_gram))
    trace_total = jnp.sum(diag_gram)
    spectral = 2.0 * square_total / (trace_total + EPS)
    gram = spread.transpose(1, 2, 0, 3).reshape(width, width)
    at_row = lax.broadcasted_iota(jnp.int32, gram.shape, 0)
    at_col = lax.broadcasted_iota(jnp.int32, gram.shape, 1)
    current = (
        jnp.where(at_row == at_col, diag_gram[:, None], gram.astype(jnp.float32)) / spectral
    )
    poly0 = (jnp.where(at_row == at_col, 1.5, 0.0) - 0.5 * current).astype(jnp.bfloat16)
    product = chain(current.astype(jnp.bfloat16), poly0, rows_dev)
    factor = jnp.sqrt(2.0 * hidden / spectral)
    ortho = jnp.dot(product, columns, preferred_element_type=jnp.float32) * factor
    half = grad_gate.shape[1]
    return (moment_gate_next, moment_up_next, ortho[:, :half], ortho[:, half:])


def solution(mesh):
    in_specs = (P("fs", "tp"), P("fs", "tp"), P("fs", "tp"), P("fs", "tp"))
    out_specs = (P("fs", "tp"), P("fs", "tp"), P("fs", "tp"), P("fs", "tp"))
    return jax.shard_map(local, mesh=mesh, in_specs=in_specs, out_specs=out_specs, check_vma=False)
```
